128 devices in a mesh: sp: 32 (over z, y, core), tp: 4 (over x).
Axes of the slice: x: 4, y: 4, z: 4, core: 2. Of those that a mesh axis runs over, the one named last changes fastest.
Arguments:
- query_nope: bfloat16 [6144, 4096], P('sp', 'tp'), may hold values from -6 to 6
- query_rope: bfloat16 [6144, 2048], P('sp', 'tp'), may hold values from -24 to 24
- latent: bfloat16 [6144, 512], P('sp'), may hold values from -6 to 6
- key_rope: bfloat16 [6144, 32], P('sp'), may hold values from -24 to 24
- latent_gain: float32 [512], replicated, may hold values from 0.1 to 1.9
- key_up: bfloat16 [512, 4096], P(None, 'tp'), may hold values from -0.25 to 0.25
- value_up: bfloat16 [512, 4096], P(None, 'tp'), may hold values from -0.25 to 0.25
- out_proj: bfloat16 [4096, 4096], P('tp'), may hold values from -0.09375 to 0.09375
- resid: bfloat16 [6144, 4096], P(('sp', 'tp')), may hold values from -6 to 6
- attn_gain: float32 [4096], replicated, may hold values from 0.1 to 1.9
- pre_gain: float32 [4096], replicated, may hold values from 0.1 to 1.9
- routes: int32 [6144, 2], P(('sp', 'tp')), may hold values from 0 to 31, all different within a row; in each aligned block of 48 rows (0 to 47, 48 to 95, ...) at most 6 rows name the same one
- route_weights: float32 [6144, 2], P(('sp', 'tp')), may hold values from 0.2 to 2
- expert_gate: bfloat16 [32, 4096, 1024], P('sp', None, 'tp'), may hold values from -0.09375 to 0.09375
- expert_up: bfloat16 [32, 4096, 1024], P('sp', None, 'tp'), may hold values from -0.09375 to 0.09375
- expert_down: bfloat16 [32, 1024, 4096], P('sp', 'tp'), may hold values from -0.1875 to 0.1875
- shared_gate: bfloat16 [4096, 1024], P(None, 'tp'), may hold values from -0.09375 to 0.09375
- shared_up: bfloat16 [4096, 1024], P(None, 'tp'), may hold values from -0.09375 to 0.09375
- shared_down: bfloat16 [1024, 4096], P('tp'), may hold values from -0.1875 to 0.1875
- moe_gain: float32 [4096], replicated, may hold values from 0.1 to 1.9
Outputs:
- output: bfloat16 [6144, 4096], P(('sp', 'tp'))
The draws below stay inside these ranges and needn't reach their ends.
Inputs may be any that keep to these rules, and one draw needn't show every extreme that they name: `routes`: A row names 2 different experts. In each aligned block of 48 rows no expert is named by more than 6 rows, and in some block an expert is named by exactly 6 rows.
All inputs are finite; a program needn't handle non-finite values.
Results may differ from the reference program's by a relative error of at most 0.018.
Values may be sent and summed in bfloat16 or wider, within the bound.
A program may use at most 128 MiB of HBM per device.

```python
import math
import jax
import jax.numpy as jnp
import numpy as np
from jax import lax

MODEL_DIM = 4096
HEADS = 64
NOPE_DIM = 64
ROPE_DIM = 32
VALUE_DIM = 64
LATENT = 512
EXPERT_FF = 1024
SHARED_FF = 1024
TOP_K = 2
ROW_DEV = 48
SEQ_LEN = 6144
EXPERTS = 32
CAPACITY = 6
N_TP = 4


def draw_query_rope(key, part):
    drawn_values = jnp.clip(jax.random.normal(jax.random.fold_in(key, 21), (SEQ_LEN, HEADS * ROPE_DIM), jnp.float32), -6.0, 6.0)
    return drawn_values.astype(jnp.bfloat16)


def draw_key_rope(key, part):
    drawn_values = jnp.clip(jax.random.normal(jax.random.fold_in(key, 22), (SEQ_LEN, ROPE_DIM), jnp.float32), -6.0, 6.0)
    return drawn_values.astype(jnp.bfloat16)


def steps_of(rng, extent, pieces, smallest, largest):
    gain = 1.0
    for dim, parts in pieces:
        draws = jax.random.uniform(jax.random.fold_in(jax.random.fold_in(rng, 6), dim), (parts,), jnp.float32, smallest / len(pieces), largest / len(pieces))
        gain = gain * jnp.repeat(jnp.exp(draws), extent[dim] // parts).reshape((-1,) + (1,) * (len(extent) - 1 - dim))
    return gain


def assign_block(stream_key, own, number, rows, amount, top, most, lean):
    ranking = jax.random.permutation(stream_key, amount)
    heavy_load, usual = load_shares(amount, rows * top, most, lean, True), load_shares(amount, rows * top, most, lean, False)
    places = jnp.arange(amount)

    def named(sizes, offset_by):
        used = int((sizes > 0).sum())
        fixed = max(1, used // 4)
        passed = fixed + (places - fixed + offset_by * (used - fixed)) % max(1, amount - fixed)
        return jnp.zeros((amount,), jnp.int32).at[ranking[jnp.where(places < fixed, places, passed)]].set(jnp.asarray(sizes, jnp.int32))

    sizes = jnp.where(number % 4 == 0, named(heavy_load, number // 4), named(usual, number - number // 4 - 1))
    mixed = jax.random.permutation(jax.random.fold_in(own, 3), amount)
    donor, taker = mixed[0:amount // 2 * 2:2], mixed[1:amount // 2 * 2:2]
    room = jnp.minimum(sizes[donor] - 1, most - sizes[taker]) // 2
    room = jnp.where((donor == ranking[0]) | (taker == ranking[0]) | (sizes[taker] == 0), 0, jnp.maximum(room, 0))
    passed = jax.random.randint(jax.random.fold_in(own, 4), (amount // 2,), 0, 1 << 20) % (room + 1)
    sizes = sizes.at[donor].add(-passed).at[taker].add(passed)
    items = jnp.searchsorted(jnp.cumsum(sizes), jnp.arange(rows * top), side="right").astype(jnp.int32)
    table = items.reshape(top, rows).T
    table = table[jax.random.permutation(jax.random.fold_in(own, 1), rows)]
    offset_by = jax.random.randint(jax.random.fold_in(own, 2), (rows, 1), 0, top)
    return jnp.take_along_axis(table, (jnp.arange(top)[None, :] + offset_by) % top, axis=1)


def load_shares(amount, total, reach, slope, full):
    weights = [(1 << 20) // math.isqrt(standing ** slope) + 1 for standing in range(1, amount + 1)]
    largest = reach if full else min(reach, max(-(-total // amount), total * weights[0] // sum(weights)))
    least = 1 if total - largest >= amount - 1 else 0
    counts, spare = [largest] + [least] * (amount - 1), total - largest - least * (amount - 1)
    while spare > 0:
        candidates = [i for i in range(1, amount) if counts[i] < largest] or [i for i in range(1, amount) if counts[i] < reach]
        mass, remaining = sum([weights[i] for i in candidates]), spare
        for i in candidates:
            extra = min(reach - counts[i], max(1, remaining * weights[i] // mass), spare)
            counts[i] = counts[i] + extra
            spare = spare - extra
    return np.array(counts)


def normal_values(own_key, dims, width, reach, pieces=(), kind=jnp.bfloat16):
    array = jax.random.normal(own_key, dims, jnp.float32) * width
    if len(pieces) > 0:
        array = steps_of(own_key, dims, pieces, -0.22, 0.18) * array
    return jnp.clip(array, min=-reach, max=reach).astype(kind)


def setup_inputs(seed: int = 0) -> dict:
    seeds = jax.random.split(jax.random.key(seed), 21)
    query_nope = normal_values(seeds[0], (SEQ_LEN, HEADS * NOPE_DIM), 1.0, 6.0, ((0, 32), (1, 4)))
    query_rope = draw_query_rope(jax.random.fold_in(seeds[20], 71), 0)
    latent = normal_values(seeds[2], (SEQ_LEN, LATENT), 1.0, 6.0, ((0, 32),))
    key_rope = draw_key_rope(jax.random.fold_in(seeds[20], 71), 0)
    latent_gain = jnp.clip(1.0 + 0.18 * jax.random.normal(seeds[4], (LATENT,), jnp.float32), 0.1, 1.9)
    key_up = normal_values(seeds[5], (LATENT, HEADS * NOPE_DIM), LATENT ** -0.5, 0.25, ((1, 4),))
    value_up = normal_values(seeds[6], (LATENT, HEADS * VALUE_DIM), LATENT ** -0.5, 0.25, ((1, 4),))
    out_proj = normal_values(seeds[7], (HEADS * VALUE_DIM, MODEL_DIM), (HEADS * VALUE_DIM) ** -0.5, 0.09375, ((0, 4),))
    resid = normal_values(seeds[8], (SEQ_LEN, MODEL_DIM), 1.0, 6.0, ((0, 128),))
    attn_gain = jnp.clip(1.0 + 0.18 * jax.random.normal(seeds[9], (MODEL_DIM,), jnp.float32), 0.1, 1.9)
    pre_gain = jnp.clip(1.0 + 0.18 * jax.random.normal(seeds[10], (MODEL_DIM,), jnp.float32), 0.1, 1.9)
    routes_keys = jax.random.split(jax.random.fold_in(seeds[11], 1), SEQ_LEN // ROW_DEV)
    routes_turns = jax.random.permutation(jax.random.fold_in(seeds[11], 3), SEQ_LEN // ROW_DEV)
    routes = jax.vmap(lambda own, number: assign_block(jax.random.fold_in(seeds[11], 2), own, number, ROW_DEV, EXPERTS, TOP_K, CAPACITY, 2))(routes_keys, routes_turns).reshape((SEQ_LEN, TOP_K))
    route_weights = jnp.clip(jnp.exp(math.log(2.0) - 2.3025851 * jax.random.uniform(seeds[12], (SEQ_LEN, TOP_K), jnp.float32) ** steps_of(seeds[12], (SEQ_LEN, TOP_K), ((0, 128),), -0.2, 0.2)), 0.2, 2.0)
    expert_gate = normal_values(seeds[13], (EXPERTS, MODEL_DIM, EXPERT_FF), MODEL_DIM ** -0.5, 0.09375, ((0, 32), (2, 4)))
    expert_up = normal_values(seeds[14], (EXPERTS, MODEL_DIM, EXPERT_FF), MODEL_DIM ** -0.5, 0.09375, ((0, 32), (2, 4)))
    expert_down = normal_values(seeds[15], (EXPERTS, EXPERT_FF, MODEL_DIM), EXPERT_FF ** -0.5, 0.1875, ((0, 32), (1, 4)))
    shared_gate = normal_values(seeds[16], (MODEL_DIM, SHARED_FF), MODEL_DIM ** -0.5, 0.09375, ((1, 4),))
    shared_up = normal_values(seeds[17], (MODEL_DIM, SHARED_FF), MODEL_DIM ** -0.5, 0.09375, ((1, 4),))
    shared_down = normal_values(seeds[18], (SHARED_FF, MODEL_DIM), SHARED_FF ** -0.5, 0.1875, ((0, 4),))
    moe_gain = jnp.clip(1.0 + 0.18 * jax.random.normal(seeds[19], (MODEL_DIM,), jnp.float32), 0.1, 1.9)
    return dict(query_nope=query_nope, query_rope=query_rope, latent=latent, key_rope=key_rope, latent_gain=latent_gain, key_up=key_up, value_up=value_up, out_proj=out_proj, resid=resid, attn_gain=attn_gain, pre_gain=pre_gain, routes=routes, route_weights=route_weights, expert_gate=expert_gate, expert_up=expert_up, expert_down=expert_down, shared_gate=shared_gate, shared_up=shared_up, shared_down=shared_down, moe_gain=moe_gain)


epsilon = 1e-06
theta_base = 10000.0

def rms_scale(values, gain_vector):
    return values * lax.rsqrt(lax.optimization_barrier(jnp.mean(values * values, axis=-1, keepdims=True)) + epsilon) * gain_vector

def rotate(values, positions):
    half_dim = values.shape[-1] // 2
    inverse = theta_base ** (-jnp.arange(half_dim, dtype=jnp.float32) / half_dim)
    angles = positions.astype(jnp.float32)[..., None] * inverse
    cosine = jnp.cos(angles)
    sine_part = jnp.sin(angles)
    first_half = values[..., :half_dim]
    second_half = values[..., half_dim:]
    return jnp.concatenate([first_half * cosine - second_half * sine_part, second_half * cosine + first_half * sine_part], axis=-1)

def quarter_product(left_rows, right_cols):
    part_cols = left_rows.shape[1] // N_TP
    result = jnp.zeros((left_rows.shape[0], right_cols.shape[1]), jnp.float32)
    for quarter in range(N_TP):
        partial_value = jnp.dot(left_rows[:, quarter * part_cols:(quarter + 1) * part_cols], right_cols[quarter * part_cols:(quarter + 1) * part_cols], preferred_element_type=jnp.float32)
        rounded = lax.optimization_barrier(partial_value.astype(jnp.bfloat16))
        result = result + rounded.astype(jnp.float32)
    return result

def reference(query_nope, query_rope, latent, key_rope, latent_gain, key_up, value_up, out_proj, resid, attn_gain, pre_gain, routes, route_weights, expert_gate, expert_up, expert_down, shared_gate, shared_up, shared_down, moe_gain):
    positions = jnp.arange(SEQ_LEN, dtype=jnp.int32)
    query_rot = rotate(query_rope.astype(jnp.float32).reshape(SEQ_LEN, HEADS, ROPE_DIM), positions[:, None]).astype(jnp.bfloat16)
    key_rot = rotate(key_rope.astype(jnp.float32), positions).astype(jnp.bfloat16)
    latent_normed = rms_scale(latent.astype(jnp.float32), latent_gain).astype(jnp.bfloat16)
    keys_all = jnp.dot(latent_normed, key_up, preferred_element_type=jnp.float32).astype(jnp.bfloat16)
    keys_all = keys_all.reshape(SEQ_LEN, HEADS, NOPE_DIM).astype(jnp.float32)
    values_all = jnp.dot(latent_normed, value_up, preferred_element_type=jnp.float32).astype(jnp.bfloat16)
    values_all = values_all.reshape(SEQ_LEN, HEADS, VALUE_DIM).astype(jnp.float32)
    query_heads = query_nope.reshape(SEQ_LEN, HEADS, NOPE_DIM).astype(jnp.float32)
    query_rot_f = query_rot.astype(jnp.float32)
    key_rot_f = key_rot.astype(jnp.float32)
    score_scale = (NOPE_DIM + ROPE_DIM) ** (-0.5)
    block_rows = math.gcd(SEQ_LEN, 256)
    outputs = []
    for first_row in range(0, SEQ_LEN, block_rows):
        last_row = first_row + block_rows
        scores = (jnp.einsum('qhd,khd->hqk', query_heads[first_row:last_row], keys_all[:last_row]) + jnp.einsum('qhr,kr->hqk', query_rot_f[first_row:last_row], key_rot_f[:last_row])) * score_scale
        allowed = jnp.arange(last_row)[None, :] <= (first_row + jnp.arange(block_rows))[:, None]
        scores = jnp.where(allowed[None], scores, -jnp.inf)
        row_max = lax.optimization_barrier(jnp.max(scores, axis=-1, keepdims=True))
        exponent = jnp.exp(scores - row_max)
        weights = exponent.astype(jnp.bfloat16).astype(jnp.float32)
        summed = jnp.einsum('hqk,khd->hqd', weights, values_all[:last_row])
        normalized = summed / lax.optimization_barrier(jnp.sum(exponent, axis=-1, keepdims=True))
        outputs.append(normalized.transpose(1, 0, 2).reshape(block_rows, HEADS * VALUE_DIM))
    attention = jnp.concatenate(outputs, axis=0).astype(jnp.bfloat16)
    projected = quarter_product(attention, out_proj)
    mixed = (resid.astype(jnp.float32) + rms_scale(projected, attn_gain)).astype(jnp.bfloat16)
    normed = rms_scale(mixed.astype(jnp.float32), pre_gain).astype(jnp.bfloat16)
    shared_hidden = (jax.nn.silu(jnp.dot(normed, shared_gate, preferred_element_type=jnp.float32)) * jnp.dot(normed, shared_up, preferred_element_type=jnp.float32)).astype(jnp.bfloat16)
    shared_out = quarter_product(shared_hidden, shared_down)
    blocks = SEQ_LEN // ROW_DEV
    flat_routes = routes.reshape(blocks, ROW_DEV * TOP_K)
    onehot = (flat_routes[..., None] == jnp.arange(EXPERTS, dtype=jnp.int32)[None, None, :]).astype(jnp.int32)
    earlier = jnp.cumsum(onehot, axis=1) - onehot
    slot_index = lax.optimization_barrier(jnp.sum(earlier * onehot, axis=-1))
    target = ((jnp.arange(blocks, dtype=jnp.int32)[:, None] * EXPERTS + flat_routes) * CAPACITY + slot_index).reshape(-1)
    source = jnp.arange(SEQ_LEN * TOP_K, dtype=jnp.int32) // TOP_K
    slot_table = jnp.zeros((blocks * EXPERTS * CAPACITY, MODEL_DIM), jnp.bfloat16).at[target].set(normed[source])
    grouped = slot_table.reshape(blocks, EXPERTS, CAPACITY, MODEL_DIM).transpose(1, 0, 2, 3)
    grouped = grouped.reshape(EXPERTS, blocks * CAPACITY, MODEL_DIM)

    def one_expert(operands):
        expert_in, gate_part, up_part, down_part = operands
        hidden = (jax.nn.silu(jnp.dot(expert_in, gate_part, preferred_element_type=jnp.float32)) * jnp.dot(expert_in, up_part, preferred_element_type=jnp.float32)).astype(jnp.bfloat16)
        return quarter_product(hidden, down_part).astype(jnp.bfloat16)
    expert_rows = lax.map(one_expert, (grouped, expert_gate, expert_up, expert_down))
    returned = expert_rows.reshape(EXPERTS, blocks, CAPACITY, MODEL_DIM).transpose(1, 0, 2, 3)
    returned = returned.reshape(blocks * EXPERTS * CAPACITY, MODEL_DIM)
    picked = returned[target].astype(jnp.float32).reshape(SEQ_LEN, TOP_K, MODEL_DIM)
    routed = lax.optimization_barrier(jnp.sum(picked * route_weights[..., None], axis=1))
    moe = shared_out + routed
    return (mixed.astype(jnp.float32) + rms_scale(moe, moe_gain)).astype(jnp.bfloat16)
```

```python
import functools
import math

import jax
import jax.numpy as jnp
from jax import lax
from jax.experimental import pallas as pl
from jax.experimental.pallas import tpu as pltpu
from jax.sharding import PartitionSpec as P

MODEL_DIM = 4096
NOPE_DIM = 64
ROPE_DIM = 32
VALUE_DIM = 64
TOP_K = 2


epsilon = 1e-06
theta_base = 10000.0


def cut_along(array, dim, count):
    before, after = (array.shape[:dim], array.shape[dim + 1 :])
    return jnp.moveaxis(array.reshape(*before, count, -1, *after), dim, 0)


def sum_at_owner(array, axis, dim):
    count = lax.axis_size(axis)
    blocks = lax.all_to_all(cut_along(array, dim, count), axis, 0, 0, tiled=True)
    return jnp.sum(blocks.astype(jnp.float32), axis=0)


def rms_scale(values, gain_vector):
    return (
        values
        * lax.rsqrt(jnp.mean(values * values, axis=-1, keepdims=True) + epsilon)
        * gain_vector
    )


def rotate(values, positions):
    half_dim = values.shape[-1] // 2
    inverse = theta_base ** (-jnp.arange(half_dim, dtype=jnp.float32) / half_dim)
    angles = positions.astype(jnp.float32)[..., None] * inverse
    cosine = jnp.cos(angles)
    sine_part = jnp.sin(angles)
    first_half = values[..., :half_dim]
    second_half = values[..., half_dim:]
    return jnp.concatenate(
        [
            first_half * cosine - second_half * sine_part,
            second_half * cosine + first_half * sine_part,
        ],
        axis=-1,
    )


def expert_block(expert_in, gate_part, up_part, down_part):
    hidden = (
        jax.nn.silu(jnp.dot(expert_in, gate_part, preferred_element_type=jnp.float32))
        * jnp.dot(expert_in, up_part, preferred_element_type=jnp.float32)
    ).astype(jnp.bfloat16)
    return jnp.dot(hidden, down_part, preferred_element_type=jnp.float32).astype(jnp.bfloat16)


def dispatch_table(normed_rows, route_rows, experts, capacity):
    row_count = normed_rows.shape[0]
    flat_routes = route_rows.reshape(-1)
    onehot = (flat_routes[:, None] == jnp.arange(experts, dtype=jnp.int32)[None, :]).astype(
        jnp.int32
    )
    earlier = jnp.cumsum(onehot, axis=0) - onehot
    target = flat_routes * capacity + jnp.sum(earlier * onehot, axis=1)
    matches = (
        target.reshape(row_count, -1)[None, :, :]
        == jnp.arange(experts * capacity, dtype=jnp.int32)[:, None, None]
    )
    spread = jnp.any(matches, axis=2).astype(jnp.bfloat16)
    slot_table = jnp.dot(spread, normed_rows, preferred_element_type=jnp.float32).astype(
        jnp.bfloat16
    )
    return (slot_table.reshape(experts, capacity, normed_rows.shape[1]), target)


BLK = 1024

def attend_kernel(index_fn, lat_ref, qn_ref, qr_ref, wk_ref, wv_ref, out_ref, kcat, vcat, qs, acc, mx, sa, sb):
    rows = qn_ref.shape[0]
    pairs = qn_ref.shape[1] // 128
    s = index_fn()
    nkeys = (s + 1) * rows
    steps = (nkeys + 2 * BLK - 1) // (2 * BLK)
    free = (s * rows) // (2 * BLK)
    c = (96 ** -0.5) * math.log2(math.e)

    def at(i):
        return pl.ds(pl.multiple_of(i * BLK, BLK), BLK)

    def prep(i, _):
        for par in range(2):
            kcat[par, at(i), 128:256] = lat_ref[at(i), 512:640]
            vcat[par, at(i), 128:256] = jnp.ones((BLK, 128), jnp.bfloat16)
        return 0

    lax.fori_loop(0, 2 * steps, prep, 0)
    lane = lax.broadcasted_iota(jnp.int32, (rows, 128), 1)

    def weights(j):
        cols = pl.ds(pl.multiple_of(j * 128, 128), 128)
        return jnp.concatenate([wk_ref[:, cols], wv_ref[:, cols]], axis=1)

    w0 = weights(0)

    def up0(i, _):
        kv = jnp.dot(lat_ref[at(i), 0:512], w0, preferred_element_type=jnp.float32).astype(jnp.bfloat16)
        kcat[0, at(i), 0:128] = kv[:, 0:128]
        vcat[0, at(i), 0:128] = kv[:, 128:256]
        return 0

    lax.fori_loop(0, 2 * steps, up0, 0)

    def one_pair(j, _):
        par = j % 2
        cols = pl.ds(pl.multiple_of(j * 128, 128), 128)
        qp = qn_ref[:, cols]
        zero = jnp.zeros_like(qp)
        g = qr_ref[:, pl.ds(pl.multiple_of((j // 2) * 128, 128), 128)]
        first = 2 * (j % 2)
        qs[0:rows, 0:128] = jnp.where(lane < 64, qp, zero)
        qs[rows:, 0:128] = jnp.where(lane >= 64, qp, zero)
        qs[0:rows, 128:256] = jnp.where(lane // 32 == first, g, zero)
        qs[rows:, 128:256] = jnp.where(lane // 32 == first + 1, g, zero)
        nxt = jnp.minimum(j + 1, pairs - 1)
        ncols = pl.ds(pl.multiple_of(nxt * 128, 128), 128)
        acc[...] = jnp.zeros_like(acc)
        mx[...] = jnp.full_like(mx, -1e30)

        def scores(i):
            return lax.dot_general(qs[...], kcat[par, at(i), :], (((1,), (1,)), ((), ())), preferred_element_type=jnp.float32)

        sa[...] = scores(0)

        def block(i, cur, other, masked):
            vb = vcat[par, at(i), :]
            w = jnp.concatenate([wk_ref[:, ncols], wv_ref[:, ncols]], axis=1)
            kv = jnp.dot(lat_ref[at(i), 0:512], w, preferred_element_type=jnp.float32).astype(jnp.bfloat16)
            snext = scores(jnp.minimum(i + 1, 2 * steps - 1))
            for half in range(2):
                rs = pl.ds(half * rows, rows)
                sc = cur[rs, :]
                if masked:
                    qpos = s * rows + lax.broadcasted_iota(jnp.int32, (rows, BLK), 0)
                    kpos = i * BLK + lax.broadcasted_iota(jnp.int32, (rows, BLK), 1)
                    sc = jnp.where(kpos <= qpos, sc, -1e30)
                old = mx[rs, :]
                new = jnp.maximum(old, jnp.max(sc, axis=1, keepdims=True))
                newc = new * c
                p = jnp.concatenate([jnp.exp2(sc[:, k * 128:(k + 1) * 128] * c - newc).astype(jnp.bfloat16) for k in range(BLK // 128)], axis=1)
                factor = jnp.exp2(old * c - newc)
                mx[rs, :] = new
                pv = jnp.dot(p, vb, preferred_element_type=jnp.float32)
                acc[rs, 0:128] = acc[rs, 0:128] * factor + pv[:, 0:128]
                acc[rs, 128:256] = acc[rs, 128:256] * factor + pv[:, 128:256]
            other[...] = snext
            kcat[1 - par, at(i), 0:128] = kv[:, 0:128]
            vcat[1 - par, at(i), 0:128] = kv[:, 128:256]

        def plain(i, _):
            block(2 * i, sa, sb, False)
            block(2 * i + 1, sb, sa, False)
            return 0

        def edge(i, _):
            block(2 * i, sa, sb, True)
            block(2 * i + 1, sb, sa, True)
            return 0

        lax.fori_loop(0, free, plain, 0)
        lax.fori_loop(free, steps, edge, 0)
        o0 = acc[0:rows, 0:128] / acc[0:rows, 128:256]
        o1 = acc[rows:, 0:128] / acc[rows:, 128:256]
        out_ref[:, cols] = jnp.where(lane < 64, o0, o1).astype(jnp.bfloat16)
        return 0

    lax.fori_loop(0, pairs, one_pair, 0)


def attend(index_fn, lat, qn, qr, wk, wv):
    rows = qn.shape[0]
    keys = lat.shape[0]
    return pl.pallas_call(
        functools.partial(attend_kernel, index_fn),
        out_shape=jax.ShapeDtypeStruct(qn.shape, jnp.bfloat16),
        in_specs=[pl.BlockSpec(memory_space=pltpu.VMEM)] * 5,
        out_specs=pl.BlockSpec(memory_space=pltpu.VMEM),
        scratch_shapes=[
            pltpu.VMEM((2, keys, 256), jnp.bfloat16),
            pltpu.VMEM((2, keys, 256), jnp.bfloat16),
            pltpu.VMEM((2 * rows, 256), jnp.bfloat16),
            pltpu.VMEM((2 * rows, 256), jnp.float32),
            pltpu.VMEM((2 * rows, 128), jnp.float32),
            pltpu.VMEM((2 * rows, BLK), jnp.float32),
            pltpu.VMEM((2 * rows, BLK), jnp.float32),
        ],
        compiler_params=pltpu.CompilerParams(vmem_limit_bytes=48 * 1024 * 1024),
        name="attend",
    )(lat, qn, qr, wk, wv)


def on_device(
    query_nope,
    query_rope,
    latent,
    key_rope,
    latent_gain,
    key_up,
    value_up,
    out_proj,
    resid,
    attn_gain,
    pre_gain,
    routes,
    route_weights,
    expert_gate,
    expert_up,
    expert_down,
    shared_gate,
    shared_up,
    shared_down,
    moe_gain,
):
    local_rows = query_nope.shape[0]
    heads_here = query_nope.shape[1] // NOPE_DIM
    query_pos = lax.axis_index("sp") * local_rows + jnp.arange(local_rows, dtype=jnp.int32)
    key_rot = rotate(key_rope.astype(jnp.float32), query_pos).astype(jnp.bfloat16)
    latent_normed = rms_scale(latent.astype(jnp.float32), latent_gain).astype(jnp.bfloat16)
    latent_all = lax.all_gather(
        jnp.concatenate([latent_normed] + [key_rot] * 4, axis=1), "sp", axis=0, tiled=True
    )
    query_rot = rotate(
        query_rope.astype(jnp.float32).reshape(local_rows, heads_here, ROPE_DIM), query_pos[:, None]
    ).astype(jnp.bfloat16)
    attention = attend(
        lambda: lax.axis_index("sp"),
        latent_all,
        query_nope,
        query_rot.reshape(local_rows, -1),
        key_up,
        value_up,
    )
    projected = sum_at_owner(
        jnp.dot(attention, out_proj, preferred_element_type=jnp.float32).astype(jnp.bfloat16),
        "tp",
        0,
    )
    mixed = (resid.astype(jnp.float32) + rms_scale(projected, attn_gain)).astype(jnp.bfloat16)
    normed = rms_scale(mixed.astype(jnp.float32), pre_gain).astype(jnp.bfloat16)
    rows_here = resid.shape[0]
    tp_count = lax.axis_size("tp")
    experts = lax.axis_size("sp")
    capacity = max(2, 2 * rows_here * TOP_K // experts)
    own_table, target = dispatch_table(normed, routes, experts, capacity)
    arrived = lax.all_to_all(own_table, "sp", split_axis=0, concat_axis=0, tiled=True)
    column = lax.all_gather(arrived[None], "tp", axis=0, tiled=True)
    group_normed = lax.all_gather(normed, "tp", axis=0, tiled=True)
    expert_out = expert_block(
        column.reshape(-1, MODEL_DIM), expert_gate[0], expert_up[0], expert_down[0]
    )
    shared_part = expert_block(group_normed, shared_gate, shared_up, shared_down)
    routed_sum, shared_sum = (
        lax.psum_scatter(
            expert_out.reshape(column.shape).astype(jnp.float32).astype(jnp.bfloat16),
            "tp",
            scatter_dimension=0,
            tiled=True,
        ).astype(jnp.float32),
        lax.psum_scatter(
            shared_part.reshape(tp_count, rows_here, MODEL_DIM)
            .astype(jnp.float32)
            .astype(jnp.bfloat16),
            "tp",
            scatter_dimension=0,
            tiled=True,
        ).astype(jnp.float32),
    )
    expert_rows = lax.all_to_all(
        routed_sum.astype(jnp.bfloat16), "sp", split_axis=1, concat_axis=1, tiled=True
    ).reshape(-1, MODEL_DIM)
    shared_out = shared_sum.reshape(rows_here, MODEL_DIM)
    picked = expert_rows[target].astype(jnp.float32).reshape(rows_here, TOP_K, MODEL_DIM)
    routed = jnp.sum(picked * route_weights[..., None], axis=1)
    moe = shared_out + routed
    return (mixed.astype(jnp.float32) + rms_scale(moe, moe_gain)).astype(jnp.bfloat16)


def solution(mesh):
    in_specs = (
        P("sp", "tp"),
        P("sp", "tp"),
        P("sp", None),
        P("sp", None),
        P(),
        P(None, "tp"),
        P(None, "tp"),
        P("tp", None),
        P(("sp", "tp"), None),
        P(),
        P(),
        P(("sp", "tp"), None),
        P(("sp", "tp"), None),
        P("sp", None, "tp"),
        P("sp", None, "tp"),
        P("sp", "tp", None),
        P(None, "tp"),
        P(None, "tp"),
        P("tp", None),
        P(),
    )
    out_specs = P(("sp", "tp"), None)
    return jax.shard_map(
        on_device, mesh=mesh, in_specs=in_specs, out_specs=out_specs, check_vma=False
    )
```

```python
import functools
import math

import jax
import jax.numpy as jnp
from jax import lax
from jax.experimental import pallas as pl
from jax.experimental.pallas import tpu as pltpu
from jax.sharding import PartitionSpec as P

MODEL_DIM = 4096
NOPE_DIM = 64
ROPE_DIM = 32
VALUE_DIM = 64
TOP_K = 2


epsilon = 1e-06
theta_base = 10000.0


def rms_scale(values, gain_vector):
    return (
        values
        * lax.rsqrt(jnp.mean(values * values, axis=-1, keepdims=True) + epsilon)
        * gain_vector
    )


def rotate(values, positions):
    half_dim = values.shape[-1] // 2
    inverse = theta_base ** (-jnp.arange(half_dim, dtype=jnp.float32) / half_dim)
    angles = positions.astype(jnp.float32)[..., None] * inverse
    cosine = jnp.cos(angles)
    sine_part = jnp.sin(angles)
    first_half = values[..., :half_dim]
    second_half = values[..., half_dim:]
    return jnp.concatenate(
        [
            first_half * cosine - second_half * sine_part,
            second_half * cosine + first_half * sine_part,
        ],
        axis=-1,
    )


BLK = 1024

def attend_kernel(index_fn, lat_ref, qn_ref, qr_ref, wk_ref, wv_ref, out_ref, kcat, vcat, qs, acc, mx, sa, sb):
    rows = qn_ref.shape[0]
    pairs = qn_ref.shape[1] // 128
    s = index_fn()
    nkeys = (s + 1) * rows
    steps = (nkeys + 2 * BLK - 1) // (2 * BLK)
    free = (s * rows) // (2 * BLK)
    c = (96 ** -0.5) * math.log2(math.e)

    def at(i):
        return pl.ds(pl.multiple_of(i * BLK, BLK), BLK)

    def prep(i, _):
        for par in range(2):
            kcat[par, at(i), 128:256] = lat_ref[at(i), 512:640]
            vcat[par, at(i), 128:256] = jnp.ones((BLK, 128), jnp.bfloat16)
        return 0

    lax.fori_loop(0, 2 * steps, prep, 0)
    lane = lax.broadcasted_iota(jnp.int32, (rows, 128), 1)

    def weights(j):
        cols = pl.ds(pl.multiple_of(j * 128, 128), 128)
        return jnp.concatenate([wk_ref[:, cols], wv_ref[:, cols]], axis=1)

    w0 = weights(0)

    def up0(i, _):
        kv = jnp.dot(lat_ref[at(i), 0:512], w0, preferred_element_type=jnp.float32).astype(jnp.bfloat16)
        kcat[0, at(i), 0:128] = kv[:, 0:128]
        vcat[0, at(i), 0:128] = kv[:, 128:256]
        return 0

    lax.fori_loop(0, 2 * steps, up0, 0)

    def one_pair(j, _):
        par = j % 2
        cols = pl.ds(pl.multiple_of(j * 128, 128), 128)
        qp = qn_ref[:, cols]
        zero = jnp.zeros_like(qp)
        g = qr_ref[:, pl.ds(pl.multiple_of((j // 2) * 128, 128), 128)]
        first = 2 * (j % 2)
        qs[0:rows, 0:128] = jnp.where(lane < 64, qp, zero)
        qs[rows:, 0:128] = jnp.where(lane >= 64, qp, zero)
        qs[0:rows, 128:256] = jnp.where(lane // 32 == first, g, zero)
        qs[rows:, 128:256] = jnp.where(lane // 32 == first + 1, g, zero)
        nxt = jnp.minimum(j + 1, pairs - 1)
        ncols = pl.ds(pl.multiple_of(nxt * 128, 128), 128)
        acc[...] = jnp.zeros_like(acc)
        mx[...] = jnp.full_like(mx, -1e30)

        def scores(i):
            return lax.dot_general(qs[...], kcat[par, at(i), :], (((1,), (1,)), ((), ())), preferred_element_type=jnp.float32)

        sa[...] = scores(0)

        def block(i, cur, other, masked):
            vb = vcat[par, at(i), :]
            w = jnp.concatenate([wk_ref[:, ncols], wv_ref[:, ncols]], axis=1)
            kv = jnp.dot(lat_ref[at(i), 0:512], w, preferred_element_type=jnp.float32).astype(jnp.bfloat16)
            snext = scores(jnp.minimum(i + 1, 2 * steps - 1))
            for half in range(2):
                rs = pl.ds(half * rows, rows)
                sc = cur[rs, :]
                if masked:
                    qpos = s * rows + lax.broadcasted_iota(jnp.int32, (rows, BLK), 0)
                    kpos = i * BLK + lax.broadcasted_iota(jnp.int32, (rows, BLK), 1)
                    sc = jnp.where(kpos <= qpos, sc, -1e30)
                old = mx[rs, :]
                new = jnp.maximum(old, jnp.max(sc, axis=1, keepdims=True))
                newc = new * c
                p = jnp.concatenate([jnp.exp2(sc[:, k * 128:(k + 1) * 128] * c - newc).astype(jnp.bfloat16) for k in range(BLK // 128)], axis=1)
                factor = jnp.exp2(old * c - newc)
                mx[rs, :] = new
                pv = jnp.dot(p, vb, preferred_element_type=jnp.float32)
                acc[rs, 0:128] = acc[rs, 0:128] * factor + pv[:, 0:128]
                acc[rs, 128:256] = acc[rs, 128:256] * factor + pv[:, 128:256]
            other[...] = snext
            kcat[1 - par, at(i), 0:128] = kv[:, 0:128]
            vcat[1 - par, at(i), 0:128] = kv[:, 128:256]

        def plain(i, _):
            block(2 * i, sa, sb, False)
            block(2 * i + 1, sb, sa, False)
            return 0

        def edge(i, _):
            block(2 * i, sa, sb, True)
            block(2 * i + 1, sb, sa, True)
            return 0

        lax.fori_loop(0, free, plain, 0)
        lax.fori_loop(free, steps, edge, 0)
        o0 = acc[0:rows, 0:128] / acc[0:rows, 128:256]
        o1 = acc[rows:, 0:128] / acc[rows:, 128:256]
        out_ref[:, cols] = jnp.where(lane < 64, o0, o1).astype(jnp.bfloat16)
        return 0

    lax.fori_loop(0, pairs, one_pair, 0)


def attend(index_fn, lat, qn, qr, wk, wv):
    rows = qn.shape[0]
    keys = lat.shape[0]
    return pl.pallas_call(
        functools.partial(attend_kernel, index_fn),
        out_shape=jax.ShapeDtypeStruct(qn.shape, jnp.bfloat16),
        in_specs=[pl.BlockSpec(memory_space=pltpu.VMEM)] * 5,
        out_specs=pl.BlockSpec(memory_space=pltpu.VMEM),
        scratch_shapes=[
            pltpu.VMEM((2, keys, 256), jnp.bfloat16),
            pltpu.VMEM((2, keys, 256), jnp.bfloat16),
            pltpu.VMEM((2 * rows, 256), jnp.bfloat16),
            pltpu.VMEM((2 * rows, 256), jnp.float32),
            pltpu.VMEM((2 * rows, 128), jnp.float32),
            pltpu.VMEM((2 * rows, BLK), jnp.float32),
            pltpu.VMEM((2 * rows, BLK), jnp.float32),
        ],
        compiler_params=pltpu.CompilerParams(vmem_limit_bytes=48 * 1024 * 1024),
        name="attend",
    )(lat, qn, qr, wk, wv)


MESH = pl.DeviceIdType.MESH
SP, TP = 32, 4
SLOTS = 24
DIRECT_OUT = 1024
DIRECT_BACK = 2048
VM = pl.BlockSpec(memory_space=pltpu.VMEM)
OFFSETS = ((0, 1), (1, 0), (0, 3), (3, 0), (0, 2), (2, 0), (1, 1), (3, 3), (1, 3), (3, 1), (1, 2), (2, 1), (3, 2), (2, 3), (2, 2))


def remote(src, dst, send, recv, device):
    return pltpu.make_async_remote_copy(
        src_ref=src, dst_ref=dst, send_sem=send, recv_sem=recv, device_id=device, device_id_type=MESH
    )


def meet_tp(s, t):
    bar = pltpu.get_barrier_semaphore()
    for j in range(1, TP):
        pl.semaphore_signal(bar, inc=1, device_id=(s, lax.rem(t + j, TP)), device_id_type=MESH)
    return bar


def meet_all(s, t):
    bar = meet_tp(s, t)

    def greet(k, carry):
        pl.semaphore_signal(bar, inc=1, device_id=(lax.rem(s + k, SP), t), device_id_type=MESH)
        return carry

    lax.fori_loop(1, SP, greet, 0)
    pl.semaphore_wait(bar, SP - 1 + TP - 1)


def peers(s, k):
    entry = lax.div(k + 1, 2) - 1
    dc = lax.rem(k + 1, 2)
    dz = jnp.int32(0)
    dy = jnp.int32(0)
    for i, (a, b) in enumerate(OFFSETS):
        dz = jnp.where(entry == i, a, dz)
        dy = jnp.where(entry == i, b, dy)
    z, y, c = lax.div(s, 8), lax.rem(lax.div(s, 2), 4), lax.rem(s, 2)
    to = lax.rem(z + dz, 4) * 8 + lax.rem(y + dy, 4) * 2 + lax.rem(c + dc, 2)
    source = lax.rem(z - dz + 4, 4) * 8 + lax.rem(y - dy + 4, 4) * 2 + lax.rem(c + dc, 2)
    return to, source


def row_norm(values, gain):
    return values * lax.rsqrt(jnp.mean(values * values, axis=-1, keepdims=True) + epsilon) * gain


def mix_kernel(part, resid, gain, pre, side, mixed, group, sides, arrive, sems):
    s, t = lax.axis_index("sp"), lax.axis_index("tp")
    pl.semaphore_wait(meet_tp(s, t), TP - 1)

    def to(j):
        return (s, lax.rem(t + j, TP))

    sums = [
        remote(part.at[lax.rem(t + j, TP)], arrive.at[t], sems.at[0, j], sems.at[1, j], to(j)) for j in range(1, TP)
    ]
    extra = [remote(side, sides.at[t], sems.at[2, j], sems.at[3, j], to(j)) for j in range(1, TP)]
    for copy in sums + extra:
        copy.start()
    sides[t] = side[...]
    total = part[t].astype(jnp.float32)
    for j in range(1, TP):
        sums[j - 1].wait_recv()
        total = total + arrive[lax.rem(t - j + TP, TP)].astype(jnp.float32)
    mix = (resid[...].astype(jnp.float32) + row_norm(total, gain[...])).astype(jnp.bfloat16)
    mixed[...] = mix
    group[t] = row_norm(mix.astype(jnp.float32), pre[...]).astype(jnp.bfloat16)
    gathers = [remote(group.at[t], group.at[t], sems.at[4, j], sems.at[5, j], to(j)) for j in range(1, TP)]
    for copy in gathers:
        copy.start()
    for copy in extra + gathers:
        copy.wait()
    for copy in sums:
        copy.wait_send()


def mix_rows(part, resid, gain, pre, side):
    rows, width = resid.shape
    return pl.pallas_call(
        mix_kernel,
        out_shape=(
            jax.ShapeDtypeStruct((rows, width), jnp.bfloat16),
            jax.ShapeDtypeStruct((TP, rows, width), jnp.bfloat16),
            jax.ShapeDtypeStruct((TP, rows, 128), jnp.float32),
        ),
        in_specs=[VM] * 5,
        out_specs=(VM, VM, VM),
        scratch_shapes=[pltpu.VMEM((TP, rows, width), jnp.bfloat16), pltpu.SemaphoreType.DMA((6, TP))],
        compiler_params=pltpu.CompilerParams(collective_id=1, has_side_effects=True),
        name="mix_rows",
    )(part, resid, gain, pre, side)


def finish_kernel(part, mixed, gain, out, arrive, sems):
    s, t = lax.axis_index("sp"), lax.axis_index("tp")
    pl.semaphore_wait(meet_tp(s, t), TP - 1)
    sums = [
        remote(part.at[lax.rem(t + j, TP)], arrive.at[t], sems.at[0, j], sems.at[1, j], (s, lax.rem(t + j, TP)))
        for j in range(1, TP)
    ]
    for copy in sums:
        copy.start()
    total = part[t].astype(jnp.float32)
    for j in range(1, TP):
        sums[j - 1].wait_recv()
        total = total + arrive[lax.rem(t - j + TP, TP)].astype(jnp.float32)
    out[...] = (mixed[...].astype(jnp.float32) + row_norm(total, gain[...])).astype(jnp.bfloat16)
    for copy in sums:
        copy.wait_send()


def finish(part, mixed, gain):
    rows, width = mixed.shape
    return pl.pallas_call(
        finish_kernel,
        out_shape=jax.ShapeDtypeStruct((rows, width), jnp.bfloat16),
        in_specs=[VM] * 3,
        out_specs=VM,
        scratch_shapes=[pltpu.VMEM((TP, rows, width), jnp.bfloat16), pltpu.SemaphoreType.DMA((2, TP))],
        compiler_params=pltpu.CompilerParams(collective_id=2, has_side_effects=True),
        name="finish",
    )(part, mixed, gain)


def dispatch_kernel(table, out, qs, qr, ds, dr, fs, fr):
    s, t = lax.axis_index("sp"), lax.axis_index("tp")
    width = table.shape[2]
    direct_cols = DIRECT_OUT
    quarter_cols = (width - direct_cols) // TP
    half = quarter_cols // 2
    right, left, far = lax.rem(t + 1, TP), lax.rem(t + 3, TP), lax.rem(t + 2, TP)

    def cols(owner, start, size):
        return pl.ds(pl.multiple_of(direct_cols + owner * quarter_cols + start, 128), size)

    mine = cols(t, 0, quarter_cols)
    meet_all(s, t)

    def quarter(k):
        to, _ = peers(s, k)
        return remote(table.at[to, :, mine], out.at[s, :, mine], qs.at[k], qr.at[k], (to, t))

    def direct(k):
        to, _ = peers(s, k)
        at = pl.ds(0, direct_cols)
        return remote(table.at[to, :, at], out.at[s, :, at], ds.at[k], dr.at[k], (to, t))

    def relay(k, lane, owner, start, size, device):
        _, source = peers(s, k)
        block = out.at[source, :, cols(owner, start, size)]
        return remote(block, block, fs.at[lane, k], fr.at[lane, k], (s, device))

    def start_quarter(k, carry):
        quarter(k).start()
        return carry

    def start_direct(k, carry):
        direct(k).start()
        return carry

    lax.fori_loop(0, SP - 1, start_quarter, 0)
    lax.fori_loop(0, SP - 1, start_direct, 0)
    out[s] = table[s]

    def first(k, carry):
        quarter(k).wait_recv()
        relay(k, 0, t, 0, quarter_cols, right).start()
        relay(k, 1, t, 0, quarter_cols, left).start()
        return carry

    def second(k, carry):
        relay(k, 0, left, 0, quarter_cols, left).wait_recv()
        relay(k, 2, left, 0, half, right).start()
        relay(k, 1, right, 0, quarter_cols, right).wait_recv()
        relay(k, 3, right, half, half, left).start()
        return carry

    def last(k, carry):
        relay(k, 2, far, 0, half, left).wait_recv()
        relay(k, 3, far, half, half, right).wait_recv()
        direct(k).wait_recv()
        direct(k).wait_send()
        quarter(k).wait_send()
        relay(k, 0, t, 0, quarter_cols, right).wait_send()
        relay(k, 1, t, 0, quarter_cols, left).wait_send()
        relay(k, 2, left, 0, half, right).wait_send()
        relay(k, 3, right, half, half, left).wait_send()
        return carry

    lax.fori_loop(0, SP - 1, first, 0)
    lax.fori_loop(0, SP - 1, second, 0)
    lax.fori_loop(0, SP - 1, last, 0)


def dispatch(table):
    dma = pltpu.SemaphoreType.DMA
    return pl.pallas_call(
        dispatch_kernel,
        out_shape=jax.ShapeDtypeStruct(table.shape, table.dtype),
        in_specs=[VM],
        out_specs=VM,
        scratch_shapes=[dma((SP,)), dma((SP,)), dma((SP,)), dma((SP,)), dma((TP, SP)), dma((TP, SP))],
        compiler_params=pltpu.CompilerParams(
            collective_id=3, has_side_effects=True, vmem_limit_bytes=32 * 1024 * 1024
        ),
        name="dispatch",
    )(table)


def bring_kernel(rows, out, arrive, summed, qs, qr, ds, dr, xs, xr):
    s, t = lax.axis_index("sp"), lax.axis_index("tp")
    direct_cols = DIRECT_BACK
    quarter_cols = (rows.shape[2] - direct_cols) // TP

    def cols(owner):
        return pl.ds(pl.multiple_of(direct_cols + owner * quarter_cols, 128), quarter_cols)

    lead, tail = pl.ds(0, direct_cols), pl.ds(direct_cols, quarter_cols)
    meet_all(s, t)

    def block(k):
        return peers(s, k)[0]

    def direct(k):
        to = block(k)
        return remote(rows.at[to, :, lead], out.at[s, :, lead], ds.at[k], dr.at[k], (to, t))

    def quarter(k):
        to = block(k)
        return remote(summed.at[to], out.at[s, :, tail], qs.at[k], qr.at[k], (to, t))

    def cross(b, j):
        owner = lax.rem(t + j, TP)
        return remote(rows.at[b, :, cols(owner)], arrive.at[j, b], xs.at[j, b], xr.at[j, b], (s, owner))

    def launch(k, carry):
        for j in (2, 1, 3):
            cross(block(k), j).start()
        direct(k).start()
        return carry

    def add_up(b):
        total = rows[b, :, cols(t)].astype(jnp.float32)
        for j in range(1, TP):
            cross(b, j).wait_recv()
            total = total + arrive[j, b].astype(jnp.float32)
        return total.astype(jnp.bfloat16)

    def forward(k, carry):
        b = block(k)
        summed[b] = add_up(b)
        quarter(k).start()
        return carry

    def last(k, carry):
        direct(k).wait()
        quarter(k).wait()
        for j in range(1, TP):
            cross(block(k), j).wait_send()
        return carry

    lax.fori_loop(0, SP - 1, launch, 0)
    for j in (2, 1, 3):
        cross(s, j).start()
    out[s, :, 0:direct_cols] = rows[s, :, 0:direct_cols]
    lax.fori_loop(0, SP - 1, forward, 0)
    out[s, :, direct_cols:] = add_up(s)
    for j in range(1, TP):
        cross(s, j).wait_send()
    lax.fori_loop(0, SP - 1, last, 0)


def bring(rows):
    quarter_cols = (rows.shape[2] - DIRECT_BACK) // TP
    dma = pltpu.SemaphoreType.DMA
    return pl.pallas_call(
        bring_kernel,
        out_shape=jax.ShapeDtypeStruct((SP, SLOTS, DIRECT_BACK + quarter_cols), rows.dtype),
        in_specs=[VM],
        out_specs=VM,
        scratch_shapes=[
            pltpu.VMEM((TP, SP, SLOTS, quarter_cols), jnp.bfloat16),
            pltpu.VMEM((SP, SLOTS, quarter_cols), jnp.bfloat16),
            dma((SP,)),
            dma((SP,)),
            dma((SP,)),
            dma((SP,)),
            dma((TP, SP)),
            dma((TP, SP)),
        ],
        compiler_params=pltpu.CompilerParams(
            collective_id=4, has_side_effects=True, vmem_limit_bytes=32 * 1024 * 1024
        ),
        name="bring",
    )(rows)


def expert_kernel(x, gate, up, down, out):
    step = 192

    def chunk(i, carry):
        at = pl.ds(pl.multiple_of(i * step, step), step)
        rows = x[at, :]
        g = jnp.dot(rows, gate[...], preferred_element_type=jnp.float32)
        u = jnp.dot(rows, up[...], preferred_element_type=jnp.float32)
        hidden = (g / (1.0 + jnp.exp(-g)) * u).astype(jnp.bfloat16)
        for n in range(4):
            cs = pl.ds(n * 1024, 1024)
            out[at, cs] = jnp.dot(hidden, down[:, cs], preferred_element_type=jnp.float32).astype(jnp.bfloat16)
        return carry

    lax.fori_loop(0, x.shape[0] // step, chunk, 0)


def expert_rows(x, gate, up, down, name):
    return pl.pallas_call(
        expert_kernel,
        out_shape=jax.ShapeDtypeStruct(x.shape, jnp.bfloat16),
        in_specs=[VM] * 4,
        out_specs=VM,
        compiler_params=pltpu.CompilerParams(vmem_limit_bytes=32 * 1024 * 1024),
        name=name,
    )(x, gate, up, down)


def on_device(
    query_nope,
    query_rope,
    latent,
    key_rope,
    latent_gain,
    key_up,
    value_up,
    out_proj,
    resid,
    attn_gain,
    pre_gain,
    routes,
    route_weights,
    expert_gate,
    expert_up,
    expert_down,
    shared_gate,
    shared_up,
    shared_down,
    moe_gain,
):
    local_rows = query_nope.shape[0]
    heads_here = query_nope.shape[1] // NOPE_DIM
    query_pos = lax.axis_index("sp") * local_rows + jnp.arange(local_rows, dtype=jnp.int32)
    key_rot = rotate(key_rope.astype(jnp.float32), query_pos).astype(jnp.bfloat16)
    latent_normed = rms_scale(latent.astype(jnp.float32), latent_gain).astype(jnp.bfloat16)
    latent_all = lax.all_gather(
        jnp.concatenate([latent_normed] + [key_rot] * 4, axis=1), "sp", axis=0, tiled=True
    )
    query_rot = rotate(
        query_rope.astype(jnp.float32).reshape(local_rows, heads_here, ROPE_DIM), query_pos[:, None]
    ).astype(jnp.bfloat16)
    attention = attend(
        lambda: lax.axis_index("sp"),
        latent_all,
        query_nope,
        query_rot.reshape(local_rows, -1),
        key_up,
        value_up,
    )
    rows_here = resid.shape[0]
    tp_index = lax.axis_index("tp")
    capacity = SLOTS // TP
    flat_routes = routes.reshape(-1)
    onehot = (flat_routes[:, None] == jnp.arange(SP, dtype=jnp.int32)[None, :]).astype(jnp.int32)
    earlier = jnp.cumsum(onehot, axis=0) - onehot
    target = flat_routes * SLOTS + tp_index * capacity + jnp.sum(earlier * onehot, axis=1)
    side = jnp.concatenate(
        [
            target.reshape(rows_here, TOP_K).astype(jnp.float32),
            route_weights,
            jnp.zeros((rows_here, 128 - 2 * TOP_K), jnp.float32),
        ],
        axis=1,
    )
    part = jnp.dot(attention, out_proj, preferred_element_type=jnp.float32).astype(jnp.bfloat16)
    mixed, group, sides = mix_rows(
        part.reshape(TP, rows_here, MODEL_DIM), resid, attn_gain[None], pre_gain[None], side
    )
    group = group.reshape(TP * rows_here, MODEL_DIM)
    sides = sides.reshape(TP * rows_here, 128)
    slots = jnp.arange(SP * SLOTS, dtype=jnp.int32).astype(jnp.float32)
    spread = ((sides[:, 0][None] == slots[:, None]) | (sides[:, 1][None] == slots[:, None])).astype(jnp.bfloat16)
    table = jnp.dot(spread, group, preferred_element_type=jnp.float32).astype(jnp.bfloat16)
    arrived = dispatch(table.reshape(SP, SLOTS, MODEL_DIM))
    expert_out = expert_rows(
        arrived.reshape(SP * SLOTS, MODEL_DIM), expert_gate[0], expert_up[0], expert_down[0], "expert"
    )
    shared_part = expert_rows(group, shared_gate, shared_up, shared_down, "shared")
    back = bring(expert_out.reshape(SP, SLOTS, MODEL_DIM)).reshape(SP * SLOTS, -1)
    picks = jnp.where(sides[:, 0:1] == slots[None], sides[:, 2:3], 0.0) + jnp.where(
        sides[:, 1:2] == slots[None], sides[:, 3:4], 0.0
    )
    high = picks.astype(jnp.bfloat16)
    low = (picks - high.astype(jnp.float32)).astype(jnp.bfloat16)
    routed = jnp.dot(high, back, preferred_element_type=jnp.float32) + jnp.dot(
        low, back, preferred_element_type=jnp.float32
    )
    lead = shared_part[:, :DIRECT_BACK].astype(jnp.float32) + routed[:, :DIRECT_BACK]
    tail = shared_part[:, DIRECT_BACK:].astype(jnp.float32) + jnp.concatenate(
        [jnp.where(tp_index == c, routed[:, DIRECT_BACK:], 0.0) for c in range(TP)], axis=1
    )
    total = jnp.concatenate([lead.astype(jnp.bfloat16), tail.astype(jnp.bfloat16)], axis=1)
    return finish(total.reshape(TP, rows_here, MODEL_DIM), mixed, moe_gain[None])


def solution(mesh):
    in_specs = (
        P("sp", "tp"),
        P("sp", "tp"),
        P("sp", None),
        P("sp", None),
        P(),
        P(None, "tp"),
        P(None, "tp"),
        P("tp", None),
        P(("sp", "tp"), None),
        P(),
        P(),
        P(("sp", "tp"), None),
        P(("sp", "tp"), None),
        P("sp", None, "tp"),
        P("sp", None, "tp"),
        P("sp", "tp", None),
        P(None, "tp"),
        P(None, "tp"),
        P("tp", None),
        P(),
    )
    out_specs = P(("sp", "tp"), None)
    return jax.shard_map(
        on_device, mesh=mesh, in_specs=in_specs, out_specs=out_specs, check_vma=False
    )
```

```python
import functools
import math

import jax
import jax.numpy as jnp
from jax import lax
from jax.experimental import pallas as pl
from jax.experimental.pallas import tpu as pltpu
from jax.sharding import PartitionSpec as P

MODEL_DIM = 4096
NOPE_DIM = 64
ROPE_DIM = 32
VALUE_DIM = 64
TOP_K = 2


epsilon = 1e-06
theta_base = 10000.0


def rms_scale(values, gain_vector):
    return (
        values
        * lax.rsqrt(jnp.mean(values * values, axis=-1, keepdims=True) + epsilon)
        * gain_vector
    )


def rotate(values, positions):
    half_dim = values.shape[-1] // 2
    inverse = theta_base ** (-jnp.arange(half_dim, dtype=jnp.float32) / half_dim)
    angles = positions.astype(jnp.float32)[..., None] * inverse
    cosine = jnp.cos(angles)
    sine_part = jnp.sin(angles)
    first_half = values[..., :half_dim]
    second_half = values[..., half_dim:]
    return jnp.concatenate(
        [
            first_half * cosine - second_half * sine_part,
            second_half * cosine + first_half * sine_part,
        ],
        axis=-1,
    )


BLK = 1024

def attend_kernel(index_fn, lat_ref, qn_ref, qr_ref, wk_ref, wv_ref, out_ref, kcat, vcat, qs, acc, mx, sa, sb):
    rows = qn_ref.shape[0]
    pairs = qn_ref.shape[1] // 128
    s = index_fn()
    nkeys = (s + 1) * rows
    steps = (nkeys + 2 * BLK - 1) // (2 * BLK)
    free = (s * rows) // (2 * BLK)
    c = (96 ** -0.5) * math.log2(math.e)

    def at(i):
        return pl.ds(pl.multiple_of(i * BLK, BLK), BLK)

    def prep(i, _):
        for par in range(2):
            kcat[par, at(i), 128:256] = lat_ref[at(i), 512:640]
            vcat[par, at(i), 128:256] = jnp.ones((BLK, 128), jnp.bfloat16)
        return 0

    lax.fori_loop(0, 2 * steps, prep, 0)
    lane = lax.broadcasted_iota(jnp.int32, (rows, 128), 1)

    def weights(j):
        cols = pl.ds(pl.multiple_of(j * 128, 128), 128)
        return jnp.concatenate([wk_ref[:, cols], wv_ref[:, cols]], axis=1)

    w0 = weights(0)

    def up0(i, _):
        kv = jnp.dot(lat_ref[at(i), 0:512], w0, preferred_element_type=jnp.float32).astype(jnp.bfloat16)
        kcat[0, at(i), 0:128] = kv[:, 0:128]
        vcat[0, at(i), 0:128] = kv[:, 128:256]
        return 0

    lax.fori_loop(0, 2 * steps, up0, 0)

    def one_pair(j, _):
        par = j % 2
        cols = pl.ds(pl.multiple_of(j * 128, 128), 128)
        qp = qn_ref[:, cols]
        zero = jnp.zeros_like(qp)
        g = qr_ref[:, pl.ds(pl.multiple_of((j // 2) * 128, 128), 128)]
        first = 2 * (j % 2)
        qs[0:rows, 0:128] = jnp.where(lane < 64, qp, zero)
        qs[rows:, 0:128] = jnp.where(lane >= 64, qp, zero)
        qs[0:rows, 128:256] = jnp.where(lane // 32 == first, g, zero)
        qs[rows:, 128:256] = jnp.where(lane // 32 == first + 1, g, zero)
        nxt = jnp.minimum(j + 1, pairs - 1)
        ncols = pl.ds(pl.multiple_of(nxt * 128, 128), 128)
        acc[...] = jnp.zeros_like(acc)
        mx[...] = jnp.full_like(mx, -1e30)

        def scores(i):
            return lax.dot_general(qs[...], kcat[par, at(i), :], (((1,), (1,)), ((), ())), preferred_element_type=jnp.float32)

        sa[...] = scores(0)

        def block(i, cur, other, masked):
            vb = vcat[par, at(i), :]
            w = jnp.concatenate([wk_ref[:, ncols], wv_ref[:, ncols]], axis=1)
            kv = jnp.dot(lat_ref[at(i), 0:512], w, preferred_element_type=jnp.float32).astype(jnp.bfloat16)
            snext = scores(jnp.minimum(i + 1, 2 * steps - 1))
            for half in range(2):
                rs = pl.ds(half * rows, rows)
                sc = cur[rs, :]
                if masked:
                    qpos = s * rows + lax.broadcasted_iota(jnp.int32, (rows, BLK), 0)
                    kpos = i * BLK + lax.broadcasted_iota(jnp.int32, (rows, BLK), 1)
                    sc = jnp.where(kpos <= qpos, sc, -1e30)
                old = mx[rs, :]
                new = jnp.maximum(old, jnp.max(sc, axis=1, keepdims=True))
                newc = new * c
                p = jnp.concatenate([jnp.exp2(sc[:, k * 128:(k + 1) * 128] * c - newc).astype(jnp.bfloat16) for k in range(BLK // 128)], axis=1)
                factor = jnp.exp2(old * c - newc)
                mx[rs, :] = new
                pv = jnp.dot(p, vb, preferred_element_type=jnp.float32)
                acc[rs, 0:128] = acc[rs, 0:128] * factor + pv[:, 0:128]
                acc[rs, 128:256] = acc[rs, 128:256] * factor + pv[:, 128:256]
            other[...] = snext
            kcat[1 - par, at(i), 0:128] = kv[:, 0:128]
            vcat[1 - par, at(i), 0:128] = kv[:, 128:256]

        def plain(i, _):
            block(2 * i, sa, sb, False)
            block(2 * i + 1, sb, sa, False)
            return 0

        def edge(i, _):
            block(2 * i, sa, sb, True)
            block(2 * i + 1, sb, sa, True)
            return 0

        lax.fori_loop(0, free, plain, 0)
        lax.fori_loop(free, steps, edge, 0)
        o0 = acc[0:rows, 0:128] / acc[0:rows, 128:256]
        o1 = acc[rows:, 0:128] / acc[rows:, 128:256]
        out_ref[:, cols] = jnp.where(lane < 64, o0, o1).astype(jnp.bfloat16)
        return 0

    lax.fori_loop(0, pairs, one_pair, 0)


def attend(index_fn, lat, qn, qr, wk, wv):
    rows = qn.shape[0]
    keys = lat.shape[0]
    return pl.pallas_call(
        functools.partial(attend_kernel, index_fn),
        out_shape=jax.ShapeDtypeStruct(qn.shape, jnp.bfloat16),
        in_specs=[pl.BlockSpec(memory_space=pltpu.VMEM)] * 5,
        out_specs=pl.BlockSpec(memory_space=pltpu.VMEM),
        scratch_shapes=[
            pltpu.VMEM((2, keys, 256), jnp.bfloat16),
            pltpu.VMEM((2, keys, 256), jnp.bfloat16),
            pltpu.VMEM((2 * rows, 256), jnp.bfloat16),
            pltpu.VMEM((2 * rows, 256), jnp.float32),
            pltpu.VMEM((2 * rows, 128), jnp.float32),
            pltpu.VMEM((2 * rows, BLK), jnp.float32),
            pltpu.VMEM((2 * rows, BLK), jnp.float32),
        ],
        compiler_params=pltpu.CompilerParams(vmem_limit_bytes=48 * 1024 * 1024),
        name="attend",
    )(lat, qn, qr, wk, wv)


MESH = pl.DeviceIdType.MESH
SP, TP = 32, 4
SLOTS = 24
DIRECT_OUT = 1024
DIRECT_BACK = 2048
VM = pl.BlockSpec(memory_space=pltpu.VMEM)
OFFSETS = ((0, 1), (1, 0), (0, 3), (3, 0), (0, 2), (2, 0), (1, 1), (3, 3), (1, 3), (3, 1), (1, 2), (2, 1), (3, 2), (2, 3), (2, 2))


def remote(src, dst, send, recv, device):
    return pltpu.make_async_remote_copy(
        src_ref=src, dst_ref=dst, send_sem=send, recv_sem=recv, device_id=device, device_id_type=MESH
    )


def meet_tp(s, t):
    bar = pltpu.get_barrier_semaphore()
    for j in range(1, TP):
        pl.semaphore_signal(bar, inc=1, device_id=(s, lax.rem(t + j, TP)), device_id_type=MESH)
    return bar


def meet_all(s, t):
    bar = meet_tp(s, t)

    def greet(k, carry):
        pl.semaphore_signal(bar, inc=1, device_id=(lax.rem(s + k, SP), t), device_id_type=MESH)
        return carry

    lax.fori_loop(1, SP, greet, 0)
    pl.semaphore_wait(bar, SP - 1 + TP - 1)


def peers(s, k):
    entry = lax.div(k + 1, 2) - 1
    dc = lax.rem(k + 1, 2)
    dz = jnp.int32(0)
    dy = jnp.int32(0)
    for i, (a, b) in enumerate(OFFSETS):
        dz = jnp.where(entry == i, a, dz)
        dy = jnp.where(entry == i, b, dy)
    z, y, c = lax.div(s, 8), lax.rem(lax.div(s, 2), 4), lax.rem(s, 2)
    to = lax.rem(z + dz, 4) * 8 + lax.rem(y + dy, 4) * 2 + lax.rem(c + dc, 2)
    source = lax.rem(z - dz + 4, 4) * 8 + lax.rem(y - dy + 4, 4) * 2 + lax.rem(c + dc, 2)
    return to, source


def row_norm(values, gain):
    return values * lax.rsqrt(jnp.mean(values * values, axis=-1, keepdims=True) + epsilon) * gain


def mix_kernel(part, resid, gain, pre, side, mixed, group, sides, arrive, sems):
    s, t = lax.axis_index("sp"), lax.axis_index("tp")
    pl.semaphore_wait(meet_tp(s, t), TP - 1)

    def to(j):
        return (s, lax.rem(t + j, TP))

    sums = [
        remote(part.at[lax.rem(t + j, TP)], arrive.at[t], sems.at[0, j], sems.at[1, j], to(j)) for j in range(1, TP)
    ]
    extra = [remote(side, sides.at[t], sems.at[2, j], sems.at[3, j], to(j)) for j in range(1, TP)]
    for copy in sums + extra:
        copy.start()
    sides[t] = side[...]
    total = part[t].astype(jnp.float32)
    for j in range(1, TP):
        sums[j - 1].wait_recv()
        total = total + arrive[lax.rem(t - j + TP, TP)].astype(jnp.float32)
    mix = (resid[...].astype(jnp.float32) + row_norm(total, gain[...])).astype(jnp.bfloat16)
    mixed[...] = mix
    group[t] = row_norm(mix.astype(jnp.float32), pre[...]).astype(jnp.bfloat16)
    gathers = [remote(group.at[t], group.at[t], sems.at[4, j], sems.at[5, j], to(j)) for j in range(1, TP)]
    for copy in gathers:
        copy.start()
    for copy in extra + gathers:
        copy.wait()
    for copy in sums:
        copy.wait_send()


def mix_rows(part, resid, gain, pre, side):
    rows, width = resid.shape
    return pl.pallas_call(
        mix_kernel,
        out_shape=(
            jax.ShapeDtypeStruct((rows, width), jnp.bfloat16),
            jax.ShapeDtypeStruct((TP, rows, width), jnp.bfloat16),
            jax.ShapeDtypeStruct((TP, rows, 128), jnp.float32),
        ),
        in_specs=[VM] * 5,
        out_specs=(VM, VM, VM),
        scratch_shapes=[pltpu.VMEM((TP, rows, width), jnp.bfloat16), pltpu.SemaphoreType.DMA((6, TP))],
        compiler_params=pltpu.CompilerParams(collective_id=1, has_side_effects=True),
        name="mix_rows",
    )(part, resid, gain, pre, side)


def finish_kernel(part, mixed, gain, out, arrive, sems):
    s, t = lax.axis_index("sp"), lax.axis_index("tp")
    pl.semaphore_wait(meet_tp(s, t), TP - 1)
    sums = [
        remote(part.at[lax.rem(t + j, TP)], arrive.at[t], sems.at[0, j], sems.at[1, j], (s, lax.rem(t + j, TP)))
        for j in range(1, TP)
    ]
    for copy in sums:
        copy.start()
    total = part[t].astype(jnp.float32)
    for j in range(1, TP):
        sums[j - 1].wait_recv()
        total = total + arrive[lax.rem(t - j + TP, TP)].astype(jnp.float32)
    out[...] = (mixed[...].astype(jnp.float32) + row_norm(total, gain[...])).astype(jnp.bfloat16)
    for copy in sums:
        copy.wait_send()


def finish(part, mixed, gain):
    rows, width = mixed.shape
    return pl.pallas_call(
        finish_kernel,
        out_shape=jax.ShapeDtypeStruct((rows, width), jnp.bfloat16),
        in_specs=[VM] * 3,
        out_specs=VM,
        scratch_shapes=[pltpu.VMEM((TP, rows, width), jnp.bfloat16), pltpu.SemaphoreType.DMA((2, TP))],
        compiler_params=pltpu.CompilerParams(collective_id=2, has_side_effects=True),
        name="finish",
    )(part, mixed, gain)


def dispatch_kernel(table, out, qs, qr, ds, dr, fs, fr):
    s, t = lax.axis_index("sp"), lax.axis_index("tp")
    width = table.shape[2]
    direct_cols = DIRECT_OUT
    quarter_cols = (width - direct_cols) // TP
    half = quarter_cols // 2
    right, left, far = lax.rem(t + 1, TP), lax.rem(t + 3, TP), lax.rem(t + 2, TP)

    def cols(owner, start, size):
        return pl.ds(pl.multiple_of(direct_cols + owner * quarter_cols + start, 128), size)

    mine = cols(t, 0, quarter_cols)
    meet_all(s, t)

    def quarter(k):
        to, _ = peers(s, k)
        return remote(table.at[to, :, mine], out.at[s, :, mine], qs.at[k], qr.at[k], (to, t))

    def direct(k):
        to, _ = peers(s, k)
        at = pl.ds(0, direct_cols)
        return remote(table.at[to, :, at], out.at[s, :, at], ds.at[k], dr.at[k], (to, t))

    def relay(k, lane, owner, start, size, device):
        _, source = peers(s, k)
        block = out.at[source, :, cols(owner, start, size)]
        return remote(block, block, fs.at[lane, k], fr.at[lane, k], (s, device))

    def start_quarter(k, carry):
        quarter(k).start()
        return carry

    def start_direct(k, carry):
        direct(k).start()
        return carry

    lax.fori_loop(0, SP - 1, start_quarter, 0)
    lax.fori_loop(0, SP - 1, start_direct, 0)
    out[s] = table[s]

    def first(k, carry):
        quarter(k).wait_recv()
        relay(k, 0, t, 0, quarter_cols, right).start()
        relay(k, 1, t, 0, quarter_cols, left).start()
        return carry

    def second(k, carry):
        relay(k, 0, left, 0, quarter_cols, left).wait_recv()
        relay(k, 2, left, 0, half, right).start()
        relay(k, 1, right, 0, quarter_cols, right).wait_recv()
        relay(k, 3, right, half, half, left).start()
        return carry

    def last(k, carry):
        relay(k, 2, far, 0, half, left).wait_recv()
        relay(k, 3, far, half, half, right).wait_recv()
        direct(k).wait_recv()
        direct(k).wait_send()
        quarter(k).wait_send()
        relay(k, 0, t, 0, quarter_cols, right).wait_send()
        relay(k, 1, t, 0, quarter_cols, left).wait_send()
        relay(k, 2, left, 0, half, right).wait_send()
        relay(k, 3, right, half, half, left).wait_send()
        return carry

    lax.fori_loop(0, SP - 1, first, 0)
    lax.fori_loop(0, SP - 1, second, 0)
    lax.fori_loop(0, SP - 1, last, 0)


def dispatch(table):
    dma = pltpu.SemaphoreType.DMA
    return pl.pallas_call(
        dispatch_kernel,
        out_shape=jax.ShapeDtypeStruct(table.shape, table.dtype),
        in_specs=[VM],
        out_specs=VM,
        scratch_shapes=[dma((SP,)), dma((SP,)), dma((SP,)), dma((SP,)), dma((TP, SP)), dma((TP, SP))],
        compiler_params=pltpu.CompilerParams(
            collective_id=3, has_side_effects=True, vmem_limit_bytes=32 * 1024 * 1024
        ),
        name="dispatch",
    )(table)


def bring_kernel(rows, out, arrive, summed, qs, qr, ds, dr, xs, xr):
    s, t = lax.axis_index("sp"), lax.axis_index("tp")
    direct_cols = DIRECT_BACK
    quarter_cols = (rows.shape[2] - direct_cols) // TP

    def cols(owner):
        return pl.ds(pl.multiple_of(direct_cols + owner * quarter_cols, 128), quarter_cols)

    lead, tail = pl.ds(0, direct_cols), pl.ds(direct_cols, quarter_cols)
    meet_all(s, t)

    def block(k):
        return peers(s, k)[0]

    def direct(k):
        to = block(k)
        return remote(rows.at[to, :, lead], out.at[s, :, lead], ds.at[k], dr.at[k], (to, t))

    def quarter(k):
        to = block(k)
        return remote(summed.at[to], out.at[s, :, tail], qs.at[k], qr.at[k], (to, t))

    def cross(b, j):
        owner = lax.rem(t + j, TP)
        return remote(rows.at[b, :, cols(owner)], arrive.at[j, b], xs.at[j, b], xr.at[j, b], (s, owner))

    def launch(k, carry):
        for j in (2, 1, 3):
            cross(block(k), j).start()
        direct(k).start()
        return carry

    def add_up(b):
        total = rows[b, :, cols(t)].astype(jnp.float32)
        for j in range(1, TP):
            cross(b, j).wait_recv()
            total = total + arrive[j, b].astype(jnp.float32)
        return total.astype(jnp.bfloat16)

    def forward(k, carry):
        b = block(k)
        summed[b] = add_up(b)
        quarter(k).start()
        return carry

    def last(k, carry):
        direct(k).wait()
        quarter(k).wait()
        for j in range(1, TP):
            cross(block(k), j).wait_send()
        return carry

    lax.fori_loop(0, SP - 1, launch, 0)
    for j in (2, 1, 3):
        cross(s, j).start()
    out[s, :, 0:direct_cols] = rows[s, :, 0:direct_cols]
    lax.fori_loop(0, SP - 1, forward, 0)
    out[s, :, direct_cols:] = add_up(s)
    for j in range(1, TP):
        cross(s, j).wait_send()
    lax.fori_loop(0, SP - 1, last, 0)


def bring(rows):
    quarter_cols = (rows.shape[2] - DIRECT_BACK) // TP
    dma = pltpu.SemaphoreType.DMA
    return pl.pallas_call(
        bring_kernel,
        out_shape=jax.ShapeDtypeStruct((SP, SLOTS, DIRECT_BACK + quarter_cols), rows.dtype),
        in_specs=[VM],
        out_specs=VM,
        scratch_shapes=[
            pltpu.VMEM((TP, SP, SLOTS, quarter_cols), jnp.bfloat16),
            pltpu.VMEM((SP, SLOTS, quarter_cols), jnp.bfloat16),
            dma((SP,)),
            dma((SP,)),
            dma((SP,)),
            dma((SP,)),
            dma((TP, SP)),
            dma((TP, SP)),
        ],
        compiler_params=pltpu.CompilerParams(
            collective_id=4, has_side_effects=True, vmem_limit_bytes=32 * 1024 * 1024
        ),
        name="bring",
    )(rows)


def gather_kernel(block, out, su, ru, sv, rv, sr, rr, sd, rd):
    s, t = lax.axis_index("sp"), lax.axis_index("tp")
    z, y, c = lax.div(s, 8), lax.rem(lax.div(s, 2), 4), lax.rem(s, 2)
    rows = block.shape[0]
    half = rows // 2
    part = half // 2
    other = 1 - c

    def index(h, u, v, core):
        zz, yy = (v, u) if h == 0 else (u, v)
        return zz * 8 + yy * 2 + core

    def here(h):
        return (y, z) if h == 0 else (z, y)

    def back(x, j):
        return lax.rem(x - j + 4, 4)

    def piece(h, u, v, core, start, size):
        return out.at[index(h, u, v, core), pl.ds(h * half + start, size), :]

    bar = pltpu.get_barrier_semaphore()
    for j in range(1, 4):
        for device in (index(0, lax.rem(y + j, 4), z, c), index(0, y, lax.rem(z + j, 4), c)):
            pl.semaphore_signal(bar, inc=1, device_id=(device, t), device_id_type=MESH)
    pl.semaphore_signal(bar, inc=1, device_id=(index(0, y, z, other), t), device_id_type=MESH)
    pl.semaphore_wait(bar, 7)

    pending = []

    def send(src, dst, ss, rs, device):
        copy = remote(src, dst, ss, rs, (device, t))
        copy.start()
        pending.append(copy)

    def wait(dst, ss, rs):
        remote(dst, dst, ss, rs, (index(0, y, z, other), t)).wait_recv()

    def own(h):
        return block.at[pl.ds(h * half, half), :]

    def share(h, a, b, src=None):
        u, v = here(h)
        dst = piece(h, back(u, a), back(v, b), c, 0, half)
        send(dst if src is None else src, dst, sd.at[h, a, b], rd.at[h, a, b], index(0, y, z, other))

    def along(h, a, src=None):
        u, v = here(h)
        dst = piece(h, back(u, a), v, c, 0, half)
        for lane, j in ((0, 1), (1, 3)):
            device = index(h, u, lax.rem(v + j, 4), c)
            send(dst if src is None else src, dst, sv.at[h, a, lane], rv.at[h, a, lane], device)

    for j in (1, 3, 2):
        for h in range(2):
            u, v = here(h)
            send(own(h), piece(h, u, v, c, 0, half), su.at[h, j], ru.at[h, j], index(h, lax.rem(u + j, 4), v, c))
    for h in range(2):
        along(h, 0, own(h))
        share(h, 0, 0, own(h))
    out[s] = block[...]
    for a in (1, 3, 2):
        for h in range(2):
            u, v = here(h)
            wait(piece(h, back(u, a), v, c, 0, half), su.at[h, a], ru.at[h, a])
            along(h, a)
            share(h, a, 0)
    for a in (0, 1, 3, 2):
        for h in range(2):
            u, v = here(h)
            for lane, j in ((0, 1), (1, 3)):
                ua, vb = back(u, a), back(v, j)
                wait(piece(h, ua, vb, c, 0, half), sv.at[h, a, lane], rv.at[h, a, lane])
                block_part = piece(h, ua, vb, c, lane * part, part)
                device = index(h, u, lax.rem(v + j, 4), c)
                send(block_part, block_part, sr.at[h, a, lane], rr.at[h, a, lane], device)
                share(h, a, j)
    for a in (0, 1, 3, 2):
        for h in range(2):
            u, v = here(h)
            for lane in range(2):
                dst = piece(h, back(u, a), back(v, 2), c, lane * part, part)
                wait(dst, sr.at[h, a, lane], rr.at[h, a, lane])
            share(h, a, 2)
    for h in range(2):
        u, v = here(h)
        for a in range(4):
            for b in range(4):
                wait(piece(h, back(u, a), back(v, b), other, 0, half), sd.at[h, a, b], rd.at[h, a, b])
    for copy in pending:
        copy.wait_send()


def gather_latents(block):
    rows, width = block.shape
    dma = pltpu.SemaphoreType.DMA
    return pl.pallas_call(
        gather_kernel,
        out_shape=jax.ShapeDtypeStruct((SP, rows, width), block.dtype),
        in_specs=[VM],
        out_specs=VM,
        scratch_shapes=[
            dma((2, 4)),
            dma((2, 4)),
            dma((2, 4, 2)),
            dma((2, 4, 2)),
            dma((2, 4, 2)),
            dma((2, 4, 2)),
            dma((2, 4, 4)),
            dma((2, 4, 4)),
        ],
        compiler_params=pltpu.CompilerParams(
            collective_id=5, has_side_effects=True, vmem_limit_bytes=32 * 1024 * 1024
        ),
        name="gather_latents",
    )(block)


def expert_kernel(x, gate, up, down, out):
    step = 192

    def chunk(i, carry):
        at = pl.ds(pl.multiple_of(i * step, step), step)
        rows = x[at, :]
        g = jnp.dot(rows, gate[...], preferred_element_type=jnp.float32)
        u = jnp.dot(rows, up[...], preferred_element_type=jnp.float32)
        hidden = (g / (1.0 + jnp.exp(-g)) * u).astype(jnp.bfloat16)
        for n in range(4):
            cs = pl.ds(n * 1024, 1024)
            out[at, cs] = jnp.dot(hidden, down[:, cs], preferred_element_type=jnp.float32).astype(jnp.bfloat16)
        return carry

    lax.fori_loop(0, x.shape[0] // step, chunk, 0)


def expert_rows(x, gate, up, down, name):
    return pl.pallas_call(
        expert_kernel,
        out_shape=jax.ShapeDtypeStruct(x.shape, jnp.bfloat16),
        in_specs=[VM] * 4,
        out_specs=VM,
        compiler_params=pltpu.CompilerParams(vmem_limit_bytes=32 * 1024 * 1024),
        name=name,
    )(x, gate, up, down)


def on_device(
    query_nope,
    query_rope,
    latent,
    key_rope,
    latent_gain,
    key_up,
    value_up,
    out_proj,
    resid,
    attn_gain,
    pre_gain,
    routes,
    route_weights,
    expert_gate,
    expert_up,
    expert_down,
    shared_gate,
    shared_up,
    shared_down,
    moe_gain,
):
    local_rows = query_nope.shape[0]
    heads_here = query_nope.shape[1] // NOPE_DIM
    query_pos = lax.axis_index("sp") * local_rows + jnp.arange(local_rows, dtype=jnp.int32)
    key_rot = rotate(key_rope.astype(jnp.float32), query_pos).astype(jnp.bfloat16)
    latent_normed = rms_scale(latent.astype(jnp.float32), latent_gain).astype(jnp.bfloat16)
    latent_all = gather_latents(jnp.concatenate([latent_normed] + [key_rot] * 4, axis=1))
    latent_all = latent_all.reshape(-1, latent_all.shape[2])
    query_rot = rotate(
        query_rope.astype(jnp.float32).reshape(local_rows, heads_here, ROPE_DIM), query_pos[:, None]
    ).astype(jnp.bfloat16)
    attention = attend(
        lambda: lax.axis_index("sp"),
        latent_all,
        query_nope,
        query_rot.reshape(local_rows, -1),
        key_up,
        value_up,
    )
    rows_here = resid.shape[0]
    tp_index = lax.axis_index("tp")
    capacity = SLOTS // TP
    flat_routes = routes.reshape(-1)
    onehot = (flat_routes[:, None] == jnp.arange(SP, dtype=jnp.int32)[None, :]).astype(jnp.int32)
    earlier = jnp.cumsum(onehot, axis=0) - onehot
    target = flat_routes * SLOTS + tp_index * capacity + jnp.sum(earlier * onehot, axis=1)
    side = jnp.concatenate(
        [
            target.reshape(rows_here, TOP_K).astype(jnp.float32),
            route_weights,
            jnp.zeros((rows_here, 128 - 2 * TOP_K), jnp.float32),
        ],
        axis=1,
    )
    part = jnp.dot(attention, out_proj, preferred_element_type=jnp.float32).astype(jnp.bfloat16)
    mixed, group, sides = mix_rows(
        part.reshape(TP, rows_here, MODEL_DIM), resid, attn_gain[None], pre_gain[None], side
    )
    group = group.reshape(TP * rows_here, MODEL_DIM)
    sides = sides.reshape(TP * rows_here, 128)
    slots = jnp.arange(SP * SLOTS, dtype=jnp.int32).astype(jnp.float32)
    spread = ((sides[:, 0][None] == slots[:, None]) | (sides[:, 1][None] == slots[:, None])).astype(jnp.bfloat16)
    table = jnp.dot(spread, group, preferred_element_type=jnp.float32).astype(jnp.bfloat16)
    arrived = dispatch(table.reshape(SP, SLOTS, MODEL_DIM))
    expert_out = expert_rows(
        arrived.reshape(SP * SLOTS, MODEL_DIM), expert_gate[0], expert_up[0], expert_down[0], "expert"
    )
    shared_part = expert_rows(group, shared_gate, shared_up, shared_down, "shared")
    back = bring(expert_out.reshape(SP, SLOTS, MODEL_DIM)).reshape(SP * SLOTS, -1)
    picks = jnp.where(sides[:, 0:1] == slots[None], sides[:, 2:3], 0.0) + jnp.where(
        sides[:, 1:2] == slots[None], sides[:, 3:4], 0.0
    )
    high = picks.astype(jnp.bfloat16)
    low = (picks - high.astype(jnp.float32)).astype(jnp.bfloat16)
    routed = jnp.dot(high, back, preferred_element_type=jnp.float32) + jnp.dot(
        low, back, preferred_element_type=jnp.float32
    )
    lead = shared_part[:, :DIRECT_BACK].astype(jnp.float32) + routed[:, :DIRECT_BACK]
    tail = shared_part[:, DIRECT_BACK:].astype(jnp.float32) + jnp.concatenate(
        [jnp.where(tp_index == c, routed[:, DIRECT_BACK:], 0.0) for c in range(TP)], axis=1
    )
    total = jnp.concatenate([lead.astype(jnp.bfloat16), tail.astype(jnp.bfloat16)], axis=1)
    return finish(total.reshape(TP, rows_here, MODEL_DIM), mixed, moe_gain[None])


def solution(mesh):
    in_specs = (
        P("sp", "tp"),
        P("sp", "tp"),
        P("sp", None),
        P("sp", None),
        P(),
        P(None, "tp"),
        P(None, "tp"),
        P("tp", None),
        P(("sp", "tp"), None),
        P(),
        P(),
        P(("sp", "tp"), None),
        P(("sp", "tp"), None),
        P("sp", None, "tp"),
        P("sp", None, "tp"),
        P("sp", "tp", None),
        P(None, "tp"),
        P(None, "tp"),
        P("tp", None),
        P(),
    )
    out_specs = P(("sp", "tp"), None)
    return jax.shard_map(
        on_device, mesh=mesh, in_specs=in_specs, out_specs=out_specs, check_vma=False
    )
```
